256 devices in a mesh: sp: 64 (over z, y, x_hi), tp: 4 (over x_lo, core).
Axes of the slice: x: 4 (x_hi: 2, x_lo: 2; x = x_hi * 2 + x_lo), y: 4, z: 8, core: 2. Of those that a mesh axis runs over, the one named last changes fastest.
Arguments:
- hidden_in: bfloat16 [49152, 4096], P('sp', 'tp'), may hold values from -16 to 16
- norm_gain: bfloat16 [2, 4096], P(None, 'tp'), may hold values from 0.099609375 to 1.8984375
- value_proj: bfloat16 [2, 4096, 1024], P(None, 'tp', 'sp'), may hold values from -0.09375 to 0.09375
- gate_proj: bfloat16 [2, 4096, 1024], P(None, 'tp', 'sp'), may hold values from -0.09375 to 0.09375
- conv_taps: bfloat16 [2, 31, 1024], P(None, None, 'tp'), may hold values from -1 to 1
- conv_bias: bfloat16 [2, 1024], P(None, 'tp'), may hold values from -3 to 3
- group_gain: bfloat16 [2, 1024], P(None, 'tp'), may hold values from 0.099609375 to 1.8984375
- group_shift: bfloat16 [2, 1024], P(None, 'tp'), may hold values from -3 to 3
- out_proj: bfloat16 [2, 1024, 4096], P(None, 'sp', 'tp'), may hold values from -0.1875 to 0.1875
Outputs:
- hidden_out: bfloat16 [49152, 4096], P('sp', 'tp')
The draws below stay inside these ranges and needn't reach their ends.
All inputs are finite; a program needn't handle non-finite values.
Results may differ from the reference program's by a relative error of at most 0.012.
Values may be sent and summed in bfloat16 or wider, within the bound.
No kernel may reach another device: no remote copies, remote signals or barrier semaphores. Data moves between devices by JAX's collectives and lax.ppermute only.
A program may use at most 128 MiB of HBM per device.

```python
import jax
import jax.numpy as jnp
from jax import lax

D = 4096
C = 1024
GROUPS = 4
WIDTH = 31
LAYERS = 2
TOKENS = 49152
N_TP = 4


def draw_hidden_in(key, part):
    first_key, second_key, third_key = jax.random.split(jax.random.fold_in(key, 11), 3)
    phase = jax.random.uniform(first_key, (), jnp.float32)
    columns = jnp.arange(D, dtype=jnp.float32) / D
    column_scale = 0.3 + 1.7 * jnp.mod(columns + phase, 1.0)
    base = jnp.clip(jax.random.normal(second_key, (TOKENS, D), jnp.float32), -6.0, 6.0)
    values = base * column_scale[None, :]
    return values.astype(jnp.bfloat16)


def levels(key, shape, shards, low, high):
    level = 1.0
    for dim, parts in shards:
        steps = jax.random.uniform(jax.random.fold_in(jax.random.fold_in(key, 6), dim), (parts,), jnp.float32, low / len(shards), high / len(shards))
        level = level * jnp.repeat(jnp.exp(steps), shape[dim] // parts).reshape((-1,) + (1,) * (len(shape) - 1 - dim))
    return level


def centred(key, shape, deviation, bound, cuts=(), kind=jnp.bfloat16):
    result = deviation * jax.random.normal(key, shape, jnp.float32)
    if cuts:
        result = result * levels(key, shape, cuts, -0.22, 0.18)
    return jnp.clip(result, -bound, bound).astype(kind)


def setup_inputs(seed: int = 0) -> dict:
    arg_keys = jax.random.split(jax.random.key(seed), 10)
    return {
        "hidden_in": draw_hidden_in(jax.random.fold_in(arg_keys[9], 71), 0),
        "norm_gain": jnp.clip(1.0 + 0.18 * jax.random.normal(arg_keys[1], (LAYERS, D), jnp.float32), 0.099609375, 1.8984375).astype(jnp.bfloat16),
        "value_proj": centred(arg_keys[2], (LAYERS, D, C), D ** -0.5, 0.09375, ((1, 4), (2, 64))),
        "gate_proj": centred(arg_keys[3], (LAYERS, D, C), D ** -0.5, 0.09375, ((1, 4), (2, 64))),
        "conv_taps": centred(arg_keys[4], (LAYERS, WIDTH, C), WIDTH ** -0.5, 1.0, ((2, 4),)),
        "conv_bias": centred(arg_keys[5], (LAYERS, C), 0.5, 3.0, ((1, 4),)),
        "group_gain": jnp.clip(1.0 + 0.18 * jax.random.normal(arg_keys[6], (LAYERS, C), jnp.float32), 0.099609375, 1.8984375).astype(jnp.bfloat16),
        "group_shift": centred(arg_keys[7], (LAYERS, C), 0.5, 3.0, ((1, 4),)),
        "out_proj": centred(arg_keys[8], (LAYERS, C, D), C ** -0.5, 0.1875, ((1, 64), (2, 4))),
    }


row_floor = 1e-06
group_floor = 1e-05

def reference(hidden_in, norm_gain, value_proj, gate_proj, conv_taps, conv_bias, group_gain, group_shift, out_proj):
    residual_rows = hidden_in
    part_width = D // N_TP
    group_size = C // GROUPS
    reach_back = WIDTH - 1
    for level in range(LAYERS):
        wide_rows = residual_rows.astype(jnp.float32)
        scale_rows = lax.rsqrt(lax.optimization_barrier(jnp.mean(wide_rows * wide_rows, axis=1, keepdims=True)) + row_floor)
        normed_rows = (wide_rows * scale_rows * norm_gain[level].astype(jnp.float32)[None, :]).astype(jnp.bfloat16)
        value_sum = jnp.zeros((TOKENS, C), jnp.float32)
        gate_sum = jnp.zeros((TOKENS, C), jnp.float32)
        for block in range(N_TP):
            left_edge = block * part_width
            piece_rows = normed_rows[:, left_edge:left_edge + part_width]
            part_value = jnp.dot(piece_rows, value_proj[level, left_edge:left_edge + part_width], preferred_element_type=jnp.float32).astype(jnp.bfloat16)
            part_gate = jnp.dot(piece_rows, gate_proj[level, left_edge:left_edge + part_width], preferred_element_type=jnp.float32).astype(jnp.bfloat16)
            part_value, part_gate = lax.optimization_barrier((part_value, part_gate))
            value_sum = value_sum + part_value.astype(jnp.float32)
            gate_sum = gate_sum + part_gate.astype(jnp.float32)
        gated = (value_sum * jax.nn.sigmoid(gate_sum)).astype(jnp.bfloat16)
        padded = jnp.pad(gated.astype(jnp.float32), ((reach_back, 0), (0, 0)))
        taps = conv_taps[level].astype(jnp.float32)
        filtered = jnp.zeros((TOKENS, C), jnp.float32) + conv_bias[level].astype(jnp.float32)[None, :]
        for offset in range(WIDTH):
            filtered = filtered + taps[offset][None, :] * padded[offset:offset + TOKENS]
        grouped = filtered.reshape(TOKENS, GROUPS, group_size)
        group_mean = lax.optimization_barrier(jnp.mean(grouped, axis=2, keepdims=True))
        centered = grouped - group_mean
        group_var = lax.optimization_barrier(jnp.mean(centered * centered, axis=2, keepdims=True))
        scaled = (centered * lax.rsqrt(group_var + group_floor)).reshape(TOKENS, C)
        scaled = scaled * group_gain[level].astype(jnp.float32)[None, :] + group_shift[level].astype(jnp.float32)[None, :]
        mixed = jax.nn.silu(scaled).astype(jnp.bfloat16)
        update = jnp.dot(mixed, out_proj[level], preferred_element_type=jnp.float32)
        residual_rows = (wide_rows + update).astype(jnp.bfloat16)
    return residual_rows
```

```python
import jax
import jax.numpy as jnp
from jax import lax
from jax.experimental import pallas as pl
from jax.experimental.pallas import tpu as pltpu
from jax.sharding import PartitionSpec as P

D = 4096
C = 1024
WIDTH = 31
NZ, NY, NX = 8, 4, 2

row_floor = 1e-06
group_floor = 1e-05
BF = jnp.bfloat16
F32 = jnp.float32


def sp_perm(move):
    pairs = []
    for z in range(NZ):
        for y in range(NY):
            for x in range(NX):
                tz, ty, tx = move(z, y, x)
                pairs.append(((z * NY + y) * NX + x, ((tz % NZ) * NY + ty % NY) * NX + tx % NX))
    return pairs


def shift_z(a, d):
    return lax.ppermute(a, "sp", sp_perm(lambda z, y, x: (z + d, y, x)))


def shift_y(a, d):
    return lax.ppermute(a, "sp", sp_perm(lambda z, y, x: (z, y + d, x)))


def swap_x(a):
    return lax.ppermute(a, "sp", sp_perm(lambda z, y, x: (z, y, x + 1)))


def swap_core(a):
    return lax.ppermute(a, "tp", [(k, k ^ 1) for k in range(4)])


def swap_chip(a):
    return lax.ppermute(a, "tp", [(k, k ^ 2) for k in range(4)])


def ring(a, shift, count, d):
    found = {0: a}
    ahead, behind = a, a
    for k in range(1, count // 2 + 1):
        ahead = shift(ahead, d)
        found[(-k * d) % count] = ahead
        if k < count // 2:
            behind = shift(behind, -d)
            found[(k * d) % count] = behind
    return [found[r] for r in range(count)]


def z_last(a, d):
    return ring(jnp.concatenate(ring(a, shift_y, NY, d), axis=0), shift_z, NZ, d)


def y_last(a, d):
    return ring(jnp.concatenate(ring(a, shift_z, NZ, d), axis=0), shift_y, NY, d)


def place_gates(slot_ref, *refs):
    out_ref = refs[-1]
    v = (refs[0:8], refs[8:16])
    g = (refs[16:20], refs[20:24])
    for r in range(NZ):
        where, low = slot_ref[0, r], slot_ref[1, r]
        for s in range(2):
            out_ref[where, 0, low, pl.ds(64 * s, 64), :] = v[s][r][...]
            for y in range(NY):
                out_ref[where, 1, low, pl.ds(64 * s + 16 * y, 16), :] = g[s][y][pl.ds(16 * r, 16), :]


def place_out(slot_ref, *refs):
    out_ref = refs[-1]
    first, second = refs[0:8], refs[8:12]
    for r in range(NZ):
        where, low = slot_ref[0, r], slot_ref[1, r]
        out_ref[where, low, pl.ds(0, 64), :] = first[r][...]
        for y in range(NY):
            out_ref[where, low, pl.ds(64 + 16 * y, 16), :] = second[y][pl.ds(16 * r, 16), :]


def placed(kernel, slots, pieces, shape):
    vmem = pl.BlockSpec(memory_space=pltpu.VMEM)
    return pl.pallas_call(
        kernel,
        out_shape=jax.ShapeDtypeStruct(shape, BF),
        in_specs=[pl.BlockSpec(memory_space=pltpu.SMEM)] + [vmem] * len(pieces),
        out_specs=vmem,
    )(slots, *pieces)


def rows_dot(rows, weights):
    return lax.dot_general(rows, weights, (((1,), (1,)), ((), ())), preferred_element_type=F32)


def depthwise(extended, taps, bias, out_len):
    wide = extended.astype(F32)
    filtered = jnp.zeros((out_len, extended.shape[1]), F32) + bias[None, :]
    for j in range(WIDTH):
        filtered = filtered + taps[j][None, :] * wide[2 + j : 2 + j + out_len]
    return filtered


def group_normed(filtered, gain, shift):
    mean = jnp.mean(filtered, axis=1, keepdims=True)
    centered = filtered - mean
    var = jnp.mean(centered * centered, axis=1, keepdims=True)
    scaled = centered * lax.rsqrt(var + group_floor) * gain[None, :] + shift[None, :]
    return jax.nn.silu(scaled).astype(BF)


def on_device(
    hidden_in,
    norm_gain,
    value_proj,
    gate_proj,
    conv_taps,
    conv_bias,
    group_gain,
    group_shift,
    out_proj,
):
    layers = norm_gain.shape[0]
    tokens = hidden_in.shape[0]
    sp, tp = lax.axis_index("sp"), lax.axis_index("tp")
    z, y, x = sp // (NY * NX), (sp // NX) % NY, sp % NX

    value_rows = jnp.swapaxes(value_proj, 1, 2)
    gate_rows = jnp.swapaxes(gate_proj, 1, 2)
    own0 = jnp.concatenate([value_rows[0], gate_rows[0]], axis=0)
    own1 = jnp.concatenate([out_proj[0], value_rows[1], gate_rows[1], out_proj[1]], axis=0)

    other0 = swap_x(own0)
    front = lax.ppermute(hidden_in[tokens - 64 :], "sp", [(s, s + 1) for s in range(NZ * NY * NX - 1)])
    other1 = swap_x(own1)

    def pair(own, other, at):
        return jnp.concatenate([own[at : at + 8], other[at : at + 8]], axis=0)

    zabs = (z + jnp.arange(NZ, dtype=jnp.int32)) % NZ
    slots = jnp.stack([((zabs // 2) % 2) ^ (tp % 2), (zabs // 4) ^ (tp // 2), zabs % 2])
    slots = jnp.stack([slots[0] * 2 + slots[1], slots[2]]).astype(jnp.int32)

    def gates(own, other, at):
        v0 = z_last(pair(own, other, at), 1)
        g0 = y_last(pair(own, other, at + 16), 1)
        v1 = z_last(pair(own, other, at + 8), -1)
        g1 = y_last(pair(own, other, at + 24), -1)
        return placed(place_gates, slots, v0 + v1 + g0 + g1, (4, 2, 2, 128, 1024))

    def outs(own, other, at, d):
        first = z_last(pair(own, other, at), d)
        second = y_last(pair(own, other, at + 8), -d)
        return placed(place_out, slots, first + second, (4, 2, 128, 1024))

    w_gates = [gates(own0, other0, 0), None]
    w_outs = [outs(own1, other1, 0, 1), None]
    w_gates[1] = gates(own1, other1, 16)
    w_outs[1] = outs(own1, other1, 48, -1)

    small = jnp.concatenate(
        [conv_taps, conv_bias[:, None], group_gain[:, None], group_shift[:, None]], axis=1
    )
    place = jnp.arange(256, dtype=jnp.int32)
    source = (
        (place // 128) * 128
        + ((place // 16 + y) % 4) * 32
        + ((place // 8 + x) % 2) * 16
        + ((place // 64) % 2) * 8
        + place % 8
    )
    chosen = (jnp.arange(256, dtype=jnp.int32)[:, None] == source[None, :]).astype(BF)
    small = lax.dot_general(
        small.reshape(layers * 34, 256), chosen, (((1,), (0,)), ((), ())), preferred_element_type=F32
    ).reshape(layers, 34, 256)

    cut = 352
    chunks = [jnp.concatenate([front, hidden_in[:cut]], axis=0), hidden_in[cut:]]
    for level in range(layers):
        gain = norm_gain[level].astype(F32)
        weights = w_gates[level].reshape(2, 1024, 1024)
        w_out = w_outs[level].reshape(1024, 1024)
        p = small[level]
        lead = 32 * (layers - level)
        tail = None
        mixed = []
        for n, rows in enumerate(chunks):
            wide = rows.astype(F32)
            squares = jnp.sum(wide * wide, axis=1)
            scaled = (wide * gain[None, :]).astype(BF)
            sent = rows_dot(scaled, weights[1]).astype(BF)
            squares = squares + swap_core(squares)
            got = swap_core(sent)
            squares = squares + swap_chip(squares)
            total = rows_dot(scaled, weights[0]) + got.astype(F32)
            got = swap_chip(total[:, 512:].astype(BF))
            total = total[:, :512] + got.astype(F32)
            scale = lax.rsqrt(squares / D + row_floor)[:, None]
            u = (total[:, :256] * scale * jax.nn.sigmoid(total[:, 256:] * scale)).astype(BF)
            if n == 0:
                row = lax.broadcasted_iota(jnp.int32, u.shape, 0)
                u = jnp.where((row >= lead) | (sp > 0), u, jnp.zeros_like(u))
                extended = u
            else:
                extended = jnp.concatenate([tail, u], axis=0)
            tail = u[u.shape[0] - 32 :]
            filtered = depthwise(extended, p[:31], p[31], extended.shape[0] - 32)
            mixed.append(group_normed(filtered, p[32], p[33]))
        following = []
        for rows, own in zip(chunks, mixed):
            near = swap_core(own)
            far = swap_chip(own)
            both = swap_core(far)
            everything = jnp.concatenate([own, far, near, both], axis=1)
            update = lax.dot_general(
                everything, w_out, (((1,), (0,)), ((), ())), preferred_element_type=F32
            )
            kept = rows[rows.shape[0] - own.shape[0] :]
            following.append((kept.astype(F32) + update).astype(BF))
        chunks = following
    return jnp.concatenate(chunks, axis=0)


def solution(mesh):
    return jax.shard_map(
        on_device,
        mesh=mesh,
        in_specs=(
            P("sp", "tp"),
            P(None, "tp"),
            P(None, "tp", "sp"),
            P(None, "tp", "sp"),
            P(None, None, "tp"),
            P(None, "tp"),
            P(None, "tp"),
            P(None, "tp"),
            P(None, "sp", "tp"),
        ),
        out_specs=P("sp", "tp"),
        check_vma=False,
    )
```

```python
import functools

import jax
import jax.numpy as jnp
from jax import lax
from jax.experimental import pallas as pl
from jax.experimental.pallas import tpu as pltpu
from jax.sharding import PartitionSpec as P


D = 4096
WIDTH = 31
NZ, NY, NX = 8, 4, 2
CUTS = (352,)

row_floor = 1e-06
group_floor = 1e-05
BF = jnp.bfloat16
F32 = jnp.float32


def shifted(a, axis, d):
    count = lax.axis_size(axis)
    return lax.ppermute(a, axis, [(k, (k + d) % count) for k in range(count)])


def swap_core(a):
    return lax.ppermute(a, "tp", [(k, k ^ 1) for k in range(4)])


def swap_chip(a):
    return lax.ppermute(a, "tp", [(k, k ^ 2) for k in range(4)])


def relay_z(a, d):
    found = {0: a}
    ahead, behind = a, a
    for k in range(1, NZ // 2 + 1):
        ahead = shifted(ahead, "z", d)
        found[(-k * d) % NZ] = ahead
        if k < NZ // 2:
            behind = shifted(behind, "z", -d)
            found[(k * d) % NZ] = behind
    return [found[r] for r in range(NZ)]


def direct_y(a):
    return [a] + [shifted(a, "y", -r) for r in range(1, NY)]


def z_last(a, d):
    return relay_z(jnp.concatenate(direct_y(a), axis=0), d)


def y_last(a, d):
    return direct_y(jnp.concatenate(relay_z(a, d), axis=0))


def from_z_arrays(refs, at, r, y):
    rows = refs[0].shape[0] // NY
    return refs[r][pl.ds(rows * y + at, 32), :]


def from_y_arrays(refs, at, r, y):
    rows = refs[0].shape[0] // NZ
    return refs[y][pl.ds(rows * r + at, 32), :]


def place_gates(at_v, at_g, slot_ref, *refs):
    keep_ref, send_ref = refs[12:]
    for r in range(NZ):
        away, far, low = slot_ref[0, r], slot_ref[1, r], slot_ref[2, r]
        for here, out_ref in enumerate((keep_ref, send_ref)):

            @pl.when(away == here)
            def _():
                for y in range(NY):
                    out_ref[far, 0, low, pl.ds(32 * y, 32), :] = from_z_arrays(refs[0:8], at_v, r, y)
                    out_ref[far, 1, low, pl.ds(32 * y, 32), :] = from_y_arrays(refs[8:12], at_g, r, y)


def place_out(at, slot_ref, *refs):
    out_ref = refs[-1]
    for r in range(NZ):
        away, far, low = slot_ref[0, r], slot_ref[1, r], slot_ref[2, r]
        for y in range(NY):
            taken = from_z_arrays if len(refs) == NZ + 1 else from_y_arrays
            out_ref[away, far, low, pl.ds(32 * y, 32), :] = taken(refs[:-1], at, r, y)


def placed(kernel, slots, pieces, shapes):
    vmem = pl.BlockSpec(memory_space=pltpu.VMEM)
    return pl.pallas_call(
        kernel,
        out_shape=[jax.ShapeDtypeStruct(shape, BF) for shape in shapes],
        in_specs=[pl.BlockSpec(memory_space=pltpu.SMEM)] + [vmem] * len(pieces),
        out_specs=[vmem] * len(shapes),
    )(slots, *pieces)


def rows_dot(rows, weights):
    return lax.dot_general(rows, weights, (((1,), (1,)), ((), ())), preferred_element_type=F32)


def depthwise(extended, taps, bias, out_len):
    wide = extended.astype(F32)
    filtered = jnp.zeros((out_len, extended.shape[1]), F32) + bias[None, :]
    for j in range(WIDTH):
        filtered = filtered + taps[j][None, :] * wide[2 + j : 2 + j + out_len]
    return filtered


def group_normed(filtered, gain, shift):
    mean = jnp.mean(filtered, axis=1, keepdims=True)
    centered = filtered - mean
    var = jnp.mean(centered * centered, axis=1, keepdims=True)
    scaled = centered * lax.rsqrt(var + group_floor) * gain[None, :] + shift[None, :]
    return jax.nn.silu(scaled).astype(BF)


def on_device(
    hidden_in,
    norm_gain,
    value_proj,
    gate_proj,
    conv_taps,
    conv_bias,
    group_gain,
    group_shift,
    out_proj,
):
    layers = norm_gain.shape[0]
    tokens = hidden_in.shape[0]
    z, y, x, tp = [lax.axis_index(name) for name in ("z", "y", "x", "tp")]
    first_place = (z == 0) & (y == 0) & (x == 0)

    value_rows = jnp.swapaxes(value_proj, 1, 2)
    gate_rows = jnp.swapaxes(gate_proj, 1, 2)
    own0 = jnp.concatenate([value_rows[0], gate_rows[0]], axis=0)
    own1 = jnp.concatenate([out_proj[0], value_rows[1], gate_rows[1], out_proj[1]], axis=0)

    other0 = shifted(own0, "x", 1)

    def pair(own, other, at):
        return [own[at : at + 16], other[at : at + 16]]

    zabs = (z + jnp.arange(NZ, dtype=jnp.int32)) % NZ

    v0_y = direct_y(jnp.concatenate(pair(own0, other0, 0), axis=0))
    first_y = y_last(jnp.concatenate(pair(own0, other0, 16), axis=0), -1)
    v0_y, own1, hidden_in, conv_taps, conv_bias, group_gain, group_shift, zabs = lax.optimization_barrier(
        (v0_y, own1, hidden_in, conv_taps, conv_bias, group_gain, group_shift, zabs)
    )
    first_z = relay_z(jnp.concatenate(v0_y, axis=0), 1)
    other1 = shifted(own1, "x", 1)
    count = NZ * NY * NX
    front = lax.ppermute(hidden_in[tokens - 64 :], ("z", "y", "x"), [(s, s + 1) for s in range(count - 1)])
    slots = jnp.stack([((zabs // 2) % 2) ^ (tp % 2), (zabs // 4) ^ (tp // 2), zabs % 2]).astype(jnp.int32)
    rest_z = z_last(jnp.concatenate(pair(own1, other1, 0) + pair(own1, other1, 16), axis=0), -1)
    around = relay_z(jnp.concatenate(pair(own1, other1, 32) + pair(own1, other1, 48), axis=0), 1)
    g1_y = direct_y(jnp.concatenate([a[:32] for a in around], axis=0))
    out1_y = direct_y(jnp.concatenate([a[32:] for a in around], axis=0))
    half = (2, 2, 2, 128, 1024)
    w_gates = [
        placed(functools.partial(place_gates, 0, 0), slots, first_z + first_y, [half, half]),
        placed(functools.partial(place_gates, 32, 0), slots, rest_z + g1_y, [half, half]),
    ]
    w_outs = [
        placed(functools.partial(place_out, 0), slots, rest_z, [half])[0],
        placed(functools.partial(place_out, 0), slots, out1_y, [half])[0],
    ]

    small = jnp.concatenate(
        [conv_taps, conv_bias[:, None], group_gain[:, None], group_shift[:, None]], axis=1
    )
    place = jnp.arange(256, dtype=jnp.int32)
    source = (
        (place // 128) * 128
        + ((place // 32 + y) % 4) * 32
        + ((place // 16 + x) % 2) * 16
        + place % 16
    )
    chosen = (jnp.arange(256, dtype=jnp.int32)[:, None] == source[None, :]).astype(BF)
    small = lax.dot_general(
        small.reshape(layers * 34, 256), chosen, (((1,), (0,)), ((), ())), preferred_element_type=F32
    ).reshape(layers, 34, 256)

    edges = [0, *CUTS, tokens]
    chunks = [hidden_in[lo:hi] for lo, hi in zip(edges, edges[1:])]
    chunks[0] = jnp.concatenate([front, chunks[0]], axis=0)
    for level in range(layers):
        gain = norm_gain[level].astype(F32)
        w_keep, w_send = [w.reshape(1024, 1024) for w in w_gates[level]]
        w_out = w_outs[level].reshape(1024, 1024)
        p = small[level]
        lead = 32 * (layers - level)
        tail = None
        following = []
        halves = []
        for rows in chunks:
            wide = rows.astype(F32)
            squares = jnp.sum(wide * wide, axis=1)
            scaled = (wide * gain[None, :]).astype(BF)
            squares = squares + swap_core(squares)
            squares = squares + swap_chip(squares)
            got = swap_core(rows_dot(scaled, w_send).astype(BF))
            total = rows_dot(scaled, w_keep) + got.astype(F32)
            passed = total[:, 512:].astype(BF)
            halves.append([squares, total[:, :512], passed, swap_chip(passed)])
        for before, after in zip(halves, halves[1:]):
            before[3] = lax.optimization_barrier((before[3], after[2]))[0]
        for n, rows in enumerate(chunks):
            squares, total, _, got = halves[n]
            total = total + got.astype(F32)
            scale = lax.rsqrt(squares / D + row_floor)[:, None]
            u = (total[:, :256] * scale * jax.nn.sigmoid(total[:, 256:] * scale)).astype(BF)
            if n == 0:
                row = lax.broadcasted_iota(jnp.int32, u.shape, 0)
                u = jnp.where((row >= lead) | ~first_place, u, jnp.zeros_like(u))
                extended = u
            else:
                extended = jnp.concatenate([tail, u], axis=0)
            tail = u[u.shape[0] - 32 :]
            filtered = depthwise(extended, p[:31], p[31], extended.shape[0] - 32)
            own = group_normed(filtered, p[32], p[33])
            far = swap_chip(own)
            near = swap_core(own)
            both = swap_core(far)
            everything = jnp.concatenate([own, far, near, both], axis=1)
            update = lax.dot_general(
                everything, w_out, (((1,), (0,)), ((), ())), preferred_element_type=F32
            )
            kept = rows[rows.shape[0] - own.shape[0] :]
            following.append((kept.astype(F32) + update).astype(BF))
        chunks = following
    return jnp.concatenate(chunks, axis=0)


def solution(mesh):
    mesh = jax.sharding.Mesh(mesh.devices.reshape(NZ, NY, NX, 4), ("z", "y", "x", "tp"))
    sp = ("z", "y", "x")

    return jax.shard_map(
        on_device,
        mesh=mesh,
        in_specs=(
            P(sp, "tp"),
            P(None, "tp"),
            P(None, "tp", sp),
            P(None, "tp", sp),
            P(None, None, "tp"),
            P(None, "tp"),
            P(None, "tp"),
            P(None, "tp"),
            P(None, sp, "tp"),
        ),
        out_specs=P(sp, "tp"),
        check_vma=False,
    )
```

```python
import functools

import jax
import jax.numpy as jnp
from jax import lax
from jax.experimental import pallas as pl
from jax.experimental.pallas import tpu as pltpu
from jax.sharding import PartitionSpec as P


D = 4096
WIDTH = 31
NZ, NY, NX = 8, 4, 2
CUTS = (352,)

row_floor = 1e-06
group_floor = 1e-05
BF = jnp.bfloat16
F32 = jnp.float32


def shifted(a, axis, d):
    count = lax.axis_size(axis)
    return lax.ppermute(a, axis, [(k, (k + d) % count) for k in range(count)])


def swap_core(a):
    return lax.ppermute(a, "tp", [(k, k ^ 1) for k in range(4)])


def swap_chip(a):
    return lax.ppermute(a, "tp", [(k, k ^ 2) for k in range(4)])


def relay_z(a, d):
    found = {0: a}
    ahead, behind = a, a
    for k in range(1, NZ // 2 + 1):
        ahead = shifted(ahead, "z", d)
        found[(-k * d) % NZ] = ahead
        if k < NZ // 2:
            behind = shifted(behind, "z", -d)
            found[(k * d) % NZ] = behind
    return [found[r] for r in range(NZ)]


def direct_y(a):
    return [a] + [shifted(a, "y", -r) for r in range(1, NY)]


def z_last(a, d):
    return relay_z(jnp.concatenate(direct_y(a), axis=0), d)


def y_last(a, d):
    return direct_y(jnp.concatenate(relay_z(a, d), axis=0))


def from_z_arrays(refs, at, r, y):
    rows = refs[0].shape[0] // NY
    return refs[r][pl.ds(rows * y + at, 32), :]


def from_y_arrays(refs, at, r, y):
    rows = refs[0].shape[0] // NZ
    return refs[y][pl.ds(rows * r + at, 32), :]


def place_gates(at_v, at_g, slot_ref, *refs):
    keep_ref, send_ref = refs[12:]
    for r in range(NZ):
        away, far, low = slot_ref[0, r], slot_ref[1, r], slot_ref[2, r]
        for here, out_ref in enumerate((keep_ref, send_ref)):

            @pl.when(away == here)
            def _():
                for y in range(NY):
                    out_ref[far, 0, low, pl.ds(32 * y, 32), :] = from_z_arrays(refs[0:8], at_v, r, y)
                    out_ref[far, 1, low, pl.ds(32 * y, 32), :] = from_y_arrays(refs[8:12], at_g, r, y)


def place_out(at, slot_ref, *refs):
    out_ref = refs[-1]
    for r in range(NZ):
        away, far, low = slot_ref[0, r], slot_ref[1, r], slot_ref[2, r]
        for y in range(NY):
            taken = from_z_arrays if len(refs) == NZ + 1 else from_y_arrays
            out_ref[away, far, low, pl.ds(32 * y, 32), :] = taken(refs[:-1], at, r, y)


def placed(kernel, slots, pieces, shapes):
    vmem = pl.BlockSpec(memory_space=pltpu.VMEM)
    return pl.pallas_call(
        kernel,
        out_shape=[jax.ShapeDtypeStruct(shape, BF) for shape in shapes],
        in_specs=[pl.BlockSpec(memory_space=pltpu.SMEM)] + [vmem] * len(pieces),
        out_specs=[vmem] * len(shapes),
    )(slots, *pieces)


def rows_dot(rows, weights):
    return lax.dot_general(rows, weights, (((1,), (1,)), ((), ())), preferred_element_type=F32)


def depthwise(extended, taps, bias, out_len):
    wide = extended.astype(F32)
    filtered = jnp.zeros((out_len, extended.shape[1]), F32) + bias[None, :]
    for j in range(WIDTH):
        filtered = filtered + taps[j][None, :] * wide[2 + j : 2 + j + out_len]
    return filtered


def group_normed(filtered, gain, shift):
    mean = jnp.mean(filtered, axis=1, keepdims=True)
    centered = filtered - mean
    var = jnp.mean(centered * centered, axis=1, keepdims=True)
    scaled = centered * lax.rsqrt(var + group_floor) * gain[None, :] + shift[None, :]
    return jax.nn.silu(scaled).astype(BF)


def on_device(
    hidden_in,
    norm_gain,
    value_proj,
    gate_proj,
    conv_taps,
    conv_bias,
    group_gain,
    group_shift,
    out_proj,
):
    layers = norm_gain.shape[0]
    tokens = hidden_in.shape[0]
    z, y, x, tp = [lax.axis_index(name) for name in ("z", "y", "x", "tp")]
    first_place = (z == 0) & (y == 0) & (x == 0)

    value_rows = jnp.swapaxes(value_proj, 1, 2)
    gate_rows = jnp.swapaxes(gate_proj, 1, 2)
    own0 = jnp.concatenate([value_rows[0], gate_rows[0]], axis=0)
    own1 = jnp.concatenate([out_proj[0], value_rows[1], gate_rows[1], out_proj[1]], axis=0)

    other0 = shifted(own0, "x", 1)

    def pair(own, other, at):
        return [own[at : at + 16], other[at : at + 16]]

    zabs = (z + jnp.arange(NZ, dtype=jnp.int32)) % NZ

    v0_y = direct_y(jnp.concatenate(pair(own0, other0, 0), axis=0))
    first_y = y_last(jnp.concatenate(pair(own0, other0, 16), axis=0), -1)
    v0_y, own1, hidden_in, conv_taps, conv_bias, group_gain, group_shift, zabs = lax.optimization_barrier(
        (v0_y, own1, hidden_in, conv_taps, conv_bias, group_gain, group_shift, zabs)
    )
    first_z = relay_z(jnp.concatenate(v0_y, axis=0), 1)
    other1 = shifted(own1, "x", 1)
    count = NZ * NY * NX
    front = lax.ppermute(hidden_in[tokens - 64 :], ("z", "y", "x"), [(s, s + 1) for s in range(count - 1)])
    slots = jnp.stack([((zabs // 2) % 2) ^ (tp % 2), (zabs // 4) ^ (tp // 2), zabs % 2]).astype(jnp.int32)
    rest_z = z_last(jnp.concatenate(pair(own1, other1, 0) + pair(own1, other1, 16), axis=0), -1)
    around = relay_z(jnp.concatenate(pair(own1, other1, 32) + pair(own1, other1, 48), axis=0), 1)
    g1_y = direct_y(jnp.concatenate([a[:32] for a in around], axis=0))
    out1_y = direct_y(jnp.concatenate([a[32:] for a in around], axis=0))
    half = (2, 2, 2, 128, 1024)
    w_gates = [
        placed(functools.partial(place_gates, 0, 0), slots, first_z + first_y, [half, half]),
        placed(functools.partial(place_gates, 32, 0), slots, rest_z + g1_y, [half, half]),
    ]
    w_outs = [
        placed(functools.partial(place_out, 0), slots, rest_z, [half])[0],
        placed(functools.partial(place_out, 0), slots, out1_y, [half])[0],
    ]

    small = jnp.concatenate(
        [conv_taps, conv_bias[:, None], group_gain[:, None], group_shift[:, None]], axis=1
    )
    place = jnp.arange(256, dtype=jnp.int32)
    source = (
        (place // 128) * 128
        + ((place // 32 + y) % 4) * 32
        + ((place // 16 + x) % 2) * 16
        + place % 16
    )
    chosen = (jnp.arange(256, dtype=jnp.int32)[:, None] == source[None, :]).astype(BF)
    small = lax.dot_general(
        small.reshape(layers * 34, 256), chosen, (((1,), (0,)), ((), ())), preferred_element_type=F32
    ).reshape(layers, 34, 256)

    edges = [0, *CUTS, tokens]
    chunks = [hidden_in[lo:hi] for lo, hi in zip(edges, edges[1:])]
    chunks[0] = jnp.concatenate([front, chunks[0]], axis=0)
    for level in range(layers):
        gain = norm_gain[level].astype(F32)
        w_keep, w_send = [w.reshape(1024, 1024) for w in w_gates[level]]
        w_out = w_outs[level].reshape(1024, 1024)
        p = small[level]
        lead = 32 * (layers - level)
        tail = None
        following = []
        halves = []
        squares = jnp.concatenate([jnp.sum(jnp.square(rows.astype(F32)), axis=1) for rows in chunks])
        squares = squares + swap_core(squares)
        squares = squares + swap_chip(squares)
        ends = [sum(rows.shape[0] for rows in chunks[:n]) for n in range(1, len(chunks))]
        all_squares = jnp.split(squares, ends)
        for n, rows in enumerate(chunks):
            squares = all_squares[n]
            scaled = (rows.astype(F32) * gain[None, :]).astype(BF)
            got = swap_core(rows_dot(scaled, w_send).astype(BF))
            total = rows_dot(scaled, w_keep) + got.astype(F32)
            passed = total[:, 512:].astype(BF)
            halves.append([squares, total[:, :512], passed, swap_chip(passed)])
        for before, after in zip(halves, halves[1:]):
            before[3] = lax.optimization_barrier((before[3], after[2]))[0]
        for n, rows in enumerate(chunks):
            squares, total, _, got = halves[n]
            total = total + got.astype(F32)
            scale = lax.rsqrt(squares / D + row_floor)[:, None]
            u = (total[:, :256] * scale * jax.nn.sigmoid(total[:, 256:] * scale)).astype(BF)
            if n == 0:
                row = lax.broadcasted_iota(jnp.int32, u.shape, 0)
                u = jnp.where((row >= lead) | ~first_place, u, jnp.zeros_like(u))
                extended = u
            else:
                extended = jnp.concatenate([tail, u], axis=0)
            tail = u[u.shape[0] - 32 :]
            filtered = depthwise(extended, p[:31], p[31], extended.shape[0] - 32)
            own = group_normed(filtered, p[32], p[33])
            far = swap_chip(own)
            near = swap_core(own)
            both = swap_core(far)
            everything = jnp.concatenate([own, far, near, both], axis=1)
            update = lax.dot_general(
                everything, w_out, (((1,), (0,)), ((), ())), preferred_element_type=F32
            )
            kept = rows[rows.shape[0] - own.shape[0] :]
            following.append((kept.astype(F32) + update).astype(BF))
        chunks = following
    return jnp.concatenate(chunks, axis=0)


def solution(mesh):
    mesh = jax.sharding.Mesh(mesh.devices.reshape(NZ, NY, NX, 4), ("z", "y", "x", "tp"))
    sp = ("z", "y", "x")

    return jax.shard_map(
        on_device,
        mesh=mesh,
        in_specs=(
            P(sp, "tp"),
            P(None, "tp"),
            P(None, "tp", sp),
            P(None, "tp", sp),
            P(None, None, "tp"),
            P(None, "tp"),
            P(None, "tp"),
            P(None, "tp"),
            P(None, sp, "tp"),
        ),
        out_specs=P(sp, "tp"),
        check_vma=False,
    )
```
